256 devices in a mesh: grp: 4 (over y, x), ep: 32 (over z), tp: 2 (over core).
Axes of the slice: x: 2, y: 2, z: 32, core: 2. Of those that a mesh axis runs over, the one named last changes fastest.
The devices are a block of a 4x8x32 slice.
Arguments:
- tokens: bfloat16 [65536, 2048], P(('grp', 'ep', 'tp')), parts along dimension 0, may hold values from -6 to 6
- norm_gain: float32 [2048], replicated, may hold values from 0.1 to 1.9
- expert_ids: int32 [65536, 4], P(('grp', 'ep', 'tp')), parts along dimension 0, may hold values from 0 to 31, all different within a row; in each aligned block of 256 rows (0 to 255, 256 to 511, ...) at most 40 rows name the same one
- gate_weights: float32 [65536, 4], P(('grp', 'ep', 'tp')), parts along dimension 0, may hold values from 0.1 to 1
- expert_gate: bfloat16 [32, 2048, 512], P('ep', None, 'tp'), may hold values from -0.125 to 0.125
- expert_up: bfloat16 [32, 2048, 512], P('ep', None, 'tp'), may hold values from -0.125 to 0.125
- expert_down: bfloat16 [32, 512, 2048], P('ep', 'tp'), may hold values from -0.25 to 0.25
- shared_gate: bfloat16 [2048, 512], replicated, may hold values from -0.125 to 0.125
- shared_up: bfloat16 [2048, 512], replicated, may hold values from -0.125 to 0.125
- shared_down: bfloat16 [512, 2048], replicated, may hold values from -0.25 to 0.25
- post_gain: float32 [2048], replicated, may hold values from 0.1 to 1.9
Outputs:
- mixed: bfloat16 [65536, 2048], P(('grp', 'ep', 'tp')), parts along dimension 0
The draws below stay inside these ranges and needn't reach their ends.
There are 4 independent parts, one for each index of `grp`. The reference program is written for one: setup_inputs(seed, part) draws one part's arguments, and reference() takes and returns one part's arrays. A program takes and returns all parts, laid end to end along the dimension named above; an argument that names none is the same for every part. Nothing has to cross between parts.
Inputs may be any that keep to these rules, and one draw needn't show every extreme that they name: `expert_ids`: each row names 4 different experts; in each device's aligned block of 256 rows no expert is named by more than 40 rows, a bound that some block reaches.
All inputs are finite; a program needn't handle non-finite values.
Results may differ from the reference program's by a relative error of at most 0.0067.
Values may be sent and summed in bfloat16 or wider, within the bound.
A program may use at most 128 MiB of HBM per device.

```python
import math
import jax
import jax.numpy as jnp
import numpy as np
from jax import lax

D = 2048
FE = 512
FS = 512
EXPERTS = 32
TOP_K = 4
TOK_DEV = 256
CAP = 40
TOKENS = 16384


def shard_levels(stream_key, dims, split, low, top_value):
    def one(axis_at, blocks):
        heights = jax.random.uniform(jax.random.fold_in(jax.random.fold_in(stream_key, 6), axis_at), (blocks,), jnp.float32, low / len(split), top_value / len(split))
        return jnp.repeat(jnp.exp(heights), dims[axis_at] // blocks).reshape((-1,) + (1,) * (len(dims) - axis_at - 1))

    level = one(*split[0])
    for cut in split[1:]:
        level = level * one(*cut)
    return level


def assign_block(rng, own, number, rows, amount, top, limit, lean):
    sequence = jax.random.permutation(rng, amount)
    heavy_load, common = load_shares(amount, rows * top, limit, lean, True), load_shares(amount, rows * top, limit, lean, False)
    places = jnp.arange(amount)

    def named(sizes, offset_by):
        used = int((sizes > 0).sum())
        fixed = max(1, used // 4)
        moved = fixed + (places - fixed + offset_by * (used - fixed)) % max(1, amount - fixed)
        return jnp.zeros((amount,), jnp.int32).at[sequence[jnp.where(places < fixed, places, moved)]].set(jnp.asarray(sizes, jnp.int32))

    sizes = jnp.where(number % 4 == 0, named(heavy_load, number // 4), named(common, number - number // 4 - 1))
    mixed = jax.random.permutation(jax.random.fold_in(own, 3), amount)
    source_of, taker = mixed[0:amount // 2 * 2:2], mixed[1:amount // 2 * 2:2]
    margin = jnp.minimum(sizes[source_of] - 1, limit - sizes[taker]) // 2
    margin = jnp.where((source_of == sequence[0]) | (taker == sequence[0]) | (sizes[taker] == 0), 0, jnp.maximum(margin, 0))
    moved = jax.random.randint(jax.random.fold_in(own, 4), (amount // 2,), 0, 1 << 20) % (margin + 1)
    sizes = sizes.at[source_of].add(-moved).at[taker].add(moved)
    items = jnp.searchsorted(jnp.cumsum(sizes), jnp.arange(rows * top), side="right").astype(jnp.int32)
    table = items.reshape(top, rows).T
    table = table[jax.random.permutation(jax.random.fold_in(own, 1), rows)]
    offset_by = jax.random.randint(jax.random.fold_in(own, 2), (rows, 1), 0, top)
    return jnp.take_along_axis(table, (jnp.arange(top)[None, :] + offset_by) % top, axis=1)


def load_shares(number_of, total, bound, skew, full):
    weights = [(1 << 20) // math.isqrt(rank ** skew) + 1 for rank in range(1, number_of + 1)]
    largest = bound if full else min(bound, max(-(-total // number_of), total * weights[0] // sum(weights)))
    least = 1 if total - largest >= number_of - 1 else 0
    holding, rest = [largest] + [least] * (number_of - 1), total - largest - least * (number_of - 1)
    while rest > 0:
        free = [i for i in range(1, number_of) if holding[i] < largest] or [i for i in range(1, number_of) if holding[i] < bound]
        pool, left = sum([weights[i] for i in free]), rest
        for i in free:
            more = min(bound - holding[i], max(1, left * weights[i] // pool), rest)
            holding[i] = holding[i] + more
            rest = rest - more
    return np.array(holding)


def gaussian(own_key, dims, scale, reach, shards=(), kind=jnp.bfloat16):
    drawn = jax.random.normal(own_key, dims, jnp.float32) * scale
    if len(shards) > 0:
        drawn = shard_levels(own_key, dims, shards, -0.22, 0.18) * drawn
    return jnp.clip(drawn, min=-reach, max=reach).astype(kind)


def setup_inputs(seed: int = 0, part: int = 0) -> dict:
    streams_of = jax.random.split(jax.random.key(seed), 12)
    own_keys = jax.random.split(jax.random.fold_in(streams_of[11], part), 12)
    tokens = gaussian(own_keys[0], (TOKENS, D), 1.0, 6.0, ((0, 64),))
    norm_gain = jnp.clip(1.0 + 0.18 * jax.random.normal(streams_of[1], (D,), jnp.float32), 0.1, 1.9)
    expert_ids_keys = jax.random.split(jax.random.fold_in(own_keys[2], 1), TOKENS // TOK_DEV)
    expert_ids_turns = jax.random.permutation(jax.random.fold_in(own_keys[2], 3), TOKENS // TOK_DEV)
    expert_ids = jax.vmap(lambda own, number: assign_block(jax.random.fold_in(own_keys[2], 2), own, number, TOK_DEV, EXPERTS, TOP_K, CAP, 1))(expert_ids_keys, expert_ids_turns).reshape((TOKENS, TOP_K))
    gate_weights = jnp.clip(jnp.exp(math.log(1.0) - 2.3025851 * jax.random.uniform(own_keys[3], (TOKENS, TOP_K), jnp.float32) ** shard_levels(own_keys[3], (TOKENS, TOP_K), ((0, 64),), -0.2, 0.2)), 0.1, 1.0)
    expert_gate = gaussian(streams_of[4], (EXPERTS, D, FE), D ** -0.5, 0.125, ((0, 32), (2, 2)))
    expert_up = gaussian(streams_of[5], (EXPERTS, D, FE), D ** -0.5, 0.125, ((0, 32), (2, 2)))
    expert_down = gaussian(streams_of[6], (EXPERTS, FE, D), FE ** -0.5, 0.25, ((0, 32), (1, 2)))
    shared_gate = gaussian(streams_of[7], (D, FS), D ** -0.5, 0.125)
    shared_up = gaussian(streams_of[8], (D, FS), D ** -0.5, 0.125)
    shared_down = gaussian(streams_of[9], (FS, D), FS ** -0.5, 0.25)
    post_gain = jnp.clip(1.0 + 0.18 * jax.random.normal(streams_of[10], (D,), jnp.float32), 0.1, 1.9)
    return dict(tokens=tokens, norm_gain=norm_gain, expert_ids=expert_ids, gate_weights=gate_weights, expert_gate=expert_gate, expert_up=expert_up, expert_down=expert_down, shared_gate=shared_gate, shared_up=shared_up, shared_down=shared_down, post_gain=post_gain)


EPS = 1e-06

def rms_scale(inputs, gain):
    mean_sq = lax.optimization_barrier(jnp.mean(inputs * inputs, axis=-1, keepdims=True))
    return inputs * lax.rsqrt(mean_sq + EPS) * gain.astype(jnp.float32)

def swiglu_out(tok_rows, w_gate, w_up, w_down):
    gate_act = jnp.dot(tok_rows, w_gate, preferred_element_type=jnp.float32)
    up_act = jnp.dot(tok_rows, w_up, preferred_element_type=jnp.float32)
    hidden = (jax.nn.silu(gate_act) * up_act).astype(jnp.bfloat16)
    return jnp.dot(hidden, w_down, preferred_element_type=jnp.float32)

def reference(tokens, norm_gain, expert_ids, gate_weights, expert_gate, expert_up, expert_down, shared_gate, shared_up, shared_down, post_gain):
    tok_total = tokens.shape[0]
    width = tokens.shape[1]
    blocks = tok_total // TOK_DEV
    normed = rms_scale(tokens.astype(jnp.float32), norm_gain).astype(jnp.bfloat16)
    ids_blocked = expert_ids.reshape(blocks, TOK_DEV * TOP_K)
    onehot = (ids_blocked[:, :, None] == jnp.arange(EXPERTS, dtype=jnp.int32)[None, None, :]).astype(jnp.int32)
    slot_index = lax.optimization_barrier(jnp.sum(jnp.cumsum(onehot, axis=1) * onehot, axis=2)) - 1
    block_index = jnp.arange(blocks, dtype=jnp.int32)[:, None]
    position = (ids_blocked * (blocks * CAP) + block_index * CAP + slot_index).reshape(-1)
    source_row = (block_index * TOK_DEV + jnp.arange(TOK_DEV * TOP_K, dtype=jnp.int32)[None, :] // TOP_K).reshape(-1)
    lookup = jnp.full((EXPERTS * blocks * CAP,), tok_total, jnp.int32).at[position].set(source_row)
    lookup = lookup.reshape(EXPERTS, blocks * CAP)
    weight_table = jnp.zeros((EXPERTS * blocks * CAP,), jnp.float32).at[position].set(gate_weights.reshape(-1))
    weight_table = weight_table.reshape(EXPERTS, blocks * CAP)
    padded = jnp.concatenate([normed, jnp.zeros((1, width), jnp.bfloat16)], axis=0)

    def add_expert(combined, inputs):
        table_rows, table_weights, w_gate, w_up, w_down = inputs
        result = swiglu_out(padded[table_rows], w_gate, w_up, w_down).astype(jnp.bfloat16)
        combined = combined.at[table_rows].add(table_weights[:, None] * result.astype(jnp.float32))
        return (combined, None)
    start = jnp.zeros((tok_total + 1, width), jnp.float32)
    combined, _ = lax.scan(add_expert, start, (lookup, weight_table, expert_gate, expert_up, expert_down))
    shared_out = swiglu_out(normed, shared_gate, shared_up, shared_down)
    combined = combined[:tok_total] + shared_out
    return rms_scale(combined, post_gain).astype(jnp.bfloat16)
```

```python
import jax
import jax.numpy as jnp
from jax import lax
from jax.experimental import pallas as pl
from jax.experimental.pallas import tpu as pltpu
from jax.sharding import PartitionSpec as P

EPS = 1e-06
STRIDE = 4
MESH = pl.DeviceIdType.MESH
F32 = jnp.float32
BF16 = jnp.bfloat16


def rms_scale(inputs, gain):
    mean_sq = jnp.mean(inputs * inputs, axis=-1, keepdims=True)
    return inputs * lax.rsqrt(mean_sq + EPS) * gain


def row_length(mesh):
    coords = [getattr(d, "coords", None) for d in mesh.devices.reshape(mesh.devices.shape[0], -1)[:, 0]]
    groups = len(coords)
    if any(c is None for c in coords):
        return 1
    across = len({c[0] for c in coords})
    return across if groups % across == 0 else 1


def silu_mul(g, u):
    return g / (1.0 + jnp.exp(-g)) * u


def dot(a, b):
    return jnp.dot(a, b, preferred_element_type=F32)


def make_kernel(groups, across, ep, blk, width, fh):
    hosts = ep // STRIDE
    half = hosts // 2
    share = width // groups
    hb = blk // 2
    full_steps = (groups - 1) // 2
    steps = groups // 2

    def kernel(
        x_ref, gate_ref, up_ref, down_ref, sg_ref, su_ref, sd_ref,
        own_ref, back_ref, wall_ref,
        xs, acc, wb, sgb, sub, sdb, part,
        disp_s, disp_r, rel_s, rel_r, ch_s, ch_r, xy_s, xy_r, dd_s, dd_r, cb_s, cb_r, ld,
    ):
        grp = lax.axis_index("grp")
        z = lax.axis_index("ep")
        core = lax.axis_index("tp")
        other = 1 - core

        def place(g):
            row, col = g // across, g % across
            return row * across + (col if across == 1 else jnp.where(row % 2 == 0, col, across - 1 - col))

        pos = place(grp)
        nxt = place(lax.rem(pos + 1, groups))
        prv = place(lax.rem(pos + groups - 1, groups))

        def zat(d):
            return lax.rem(z + d + ep, ep)

        own_w = (gate_ref, up_ref, down_ref)
        peers = [{"ep": zat(d)} for d in (1, -1, 2, -2, STRIDE, -STRIDE)]
        peers += [{"tp": other}]
        if groups > 1:
            peers += [{"grp": nxt}, {"grp": prv}]
        barrier = pltpu.get_barrier_semaphore()
        for peer in peers:
            pl.semaphore_signal(barrier, inc=1, device_id=peer, device_id_type=MESH)
        pl.semaphore_wait(barrier, len(peers))

        def remote(src, dst, s, r, to):
            return pltpu.make_async_remote_copy(
                src_ref=src, dst_ref=dst, send_sem=s, recv_sem=r, device_id=to, device_id_type=MESH
            )

        sent = []

        def go(copy):
            copy.start()
            sent.append(copy)

        def dispatch(d, h):
            rows = pl.ds(h * hb, hb)
            return remote(
                x_ref.at[rows], xs.at[1 + d, rows], disp_s.at[d, h], disp_r.at[d, h],
                {"ep": zat(1 - 2 * d)},
            )

        def relay(d):
            rows = pl.ds(d * hb, hb)
            return remote(
                xs.at[1 + d, rows], xs.at[3, rows], rel_s.at[d], rel_r.at[d], {"ep": zat(1 - 2 * d)}
            )

        def slot_of(d, t):
            return t if d == 0 else hosts - t

        def rows_of(region, d, cut):
            if not cut:
                return pl.ds(region * share, share)
            return pl.ds(region * share + d * (share // 2), share // 2)

        def chain(d, m, t):
            rows = rows_of(pos, d, t == half)
            src = own_w[m].at[rows] if t == 1 else wall_ref.at[slot_of(d, t - 1), m, core, rows]
            return remote(
                src, wall_ref.at[slot_of(d, t), m, core, rows], ch_s.at[d, m, t - 1],
                ch_r.at[d, m, t - 1], {"ep": zat(STRIDE * (1 - 2 * d))},
            )

        def exchange(slot, m, j, d, cut, arriving):
            back = j if arriving else j - 1
            region = lax.rem(pos + (groups - back if d == 0 else back), groups)
            rows = rows_of(region, d, cut)
            ref = wall_ref.at[slot, m, core, rows]
            return remote(
                ref, ref, xy_s.at[slot, m, j - 1, d], xy_r.at[slot, m, j - 1, d],
                {"grp": nxt if d == 0 else prv},
            )

        def swap(slot, m):
            dst = wall_ref.at[slot, m, core]
            src = own_w[m] if slot == 0 else dst
            return remote(src, dst, dd_s.at[slot, m], dd_r.at[slot, m], {"tp": other})

        for h in range(2):
            for d in range(2):
                go(dispatch(d, h if d == 0 else 1 - h))
        for m in range(3):
            for d in range(2):
                go(chain(d, m, 1))
        for m in range(3):
            go(swap(0, m))

        loads = [
            pltpu.make_async_copy(a, b, ld.at[i])
            for i, (a, b) in enumerate(((sg_ref, sgb), (su_ref, sub), (sd_ref, sdb)))
        ]
        loads += [pltpu.make_async_copy(own_w[m], wb.at[m, core], ld.at[3 + m]) for m in range(3)]
        for load in loads:
            load.start()
        xs[0] = x_ref[...]
        for b in range(1, 4):
            acc[b] = jnp.zeros((blk, width), F32)
        for load in loads[:3]:
            load.wait()

        def shared():
            x = xs[0, :, :width]
            h = silu_mul(dot(x, sgb[...]), dot(x, sub[...])).astype(BF16)

            @pl.loop(0, width // fh)
            def _(j):
                cols = pl.ds(pl.multiple_of(j * fh, fh), fh)
                acc[0, :, cols] = dot(h, sdb[:, cols])

        shared()

        for d in range(2):
            dispatch(d, d).wait_recv()
            go(relay(d))
        for d in range(2):
            dispatch(d, 1 - d).wait_recv()
        for load in loads[3:]:
            load.wait()

        def block(slot, b, dst=None):
            expert = lax.rem(z + ep - STRIDE * slot, ep)
            x = xs[b, :, :width]
            lane = lax.broadcasted_iota(jnp.int32, (blk, 128), 1)
            pick = (lane < 3 * ep) & (lane % ep == expert)
            w = jnp.sum(jnp.where(pick, xs[b, :, width:].astype(F32), 0.0), axis=1, keepdims=True)
            hidden = [
                (silu_mul(dot(x, wb[0, c]), dot(x, wb[1, c])) * w).astype(BF16) for c in range(2)
            ]
            for j in range(width // fh):
                cols = slice(j * fh, (j + 1) * fh)
                total = acc[b, :, cols] + (
                    dot(hidden[0], wb[2, 0, cols, :]) + dot(hidden[1], wb[2, 1, cols, :])
                )
                if dst is None:
                    acc[b, :, cols] = total
                else:
                    dst[:, cols] = total.astype(dst.dtype)

        def compute(slot):
            @pl.loop(0, 4)
            def _(b):
                block(slot, b)

        def load_slot(slot):
            for m in range(3):
                swap(slot, m).wait_recv()
            copy = pltpu.make_async_copy(wall_ref.at[slot], wb, ld.at[0])
            copy.start()
            copy.wait()

        for m in range(3):
            swap(0, m).wait_recv()
        theirs = [
            pltpu.make_async_copy(wall_ref.at[0, m, other], wb.at[m, other], ld.at[m]) for m in range(3)
        ]
        for load in theirs:
            load.start()
        for load in theirs:
            load.wait()
        for d in range(2):
            relay(d).wait_recv()
        compute(0)

        ready = []
        for t in range(1, half + 1):
            slots = [slot_of(0, t)] if t == half else [slot_of(0, t), slot_of(1, t)]
            for m in range(3):
                for d in range(2):
                    chain(d, m, t).wait_recv()
                    if t < half:
                        go(chain(d, m, t + 1))
                cuts = [False] * full_steps + [True] * (steps - full_steps)
                for j, cut in enumerate(cuts, 1):
                    for slot in slots:
                        for d in range(2):
                            if j > 1:
                                exchange(slot, m, j - 1, d, cuts[j - 2], True).wait_recv()
                        for d in range(2):
                            go(exchange(slot, m, j, d, cut, False))
                    if j == 1 and ready:
                        done = ready.pop(0)
                        load_slot(done)
                        compute(done)
                for slot in slots:
                    for d in range(2):
                        if steps:
                            exchange(slot, m, steps, d, cuts[-1], True).wait_recv()
                    go(swap(slot, m))
            ready += slots
        while len(ready) > 1:
            done = ready.pop(0)
            load_slot(done)
            compute(done)

        last = ready.pop(0)
        load_slot(last)

        def combine(i):
            if i < 2:
                return remote(
                    part.at[i], back_ref.at[i], cb_s.at[i], cb_r.at[i], {"ep": zat(-1 if i == 0 else 1)}
                )
            rows = pl.ds((i - 2) * hb, hb)
            return remote(
                part.at[2, rows], back_ref.at[2, rows], cb_s.at[i], cb_r.at[i],
                {"ep": zat(-2 if i == 2 else 2)},
            )

        block(last, 3, part.at[2])
        block(last, 1, part.at[0])
        go(combine(2))
        go(combine(3))
        block(last, 2, part.at[1])
        go(combine(0))
        block(last, 0, own_ref)
        go(combine(1))
        for i in range(4):
            combine(i).wait_recv()
        for copy in sent:
            copy.wait_send()

    dma = pltpu.SemaphoreType.DMA
    nsteps = max(steps, 1)
    scratch = [
        pltpu.VMEM((4, blk, width + 128), BF16),
        pltpu.VMEM((4, blk, width), F32),
        pltpu.VMEM((3, 2, width, fh), BF16),
        pltpu.VMEM((width, 2 * fh), BF16),
        pltpu.VMEM((width, 2 * fh), BF16),
        pltpu.VMEM((2 * fh, width), BF16),
        pltpu.VMEM((3, blk, width), BF16),
        dma((2, 2)), dma((2, 2)), dma((2,)), dma((2,)),
        dma((2, 3, half)), dma((2, 3, half)),
        dma((hosts, 3, nsteps, 2)), dma((hosts, 3, nsteps, 2)),
        dma((hosts, 3)), dma((hosts, 3)),
        dma((4,)), dma((4,)),
        dma((6,)),
    ]
    anywhere = pl.BlockSpec(memory_space=pl.ANY)
    vmem = pl.BlockSpec(memory_space=pltpu.VMEM)
    return pl.pallas_call(
        kernel,
        out_shape=(
            jax.ShapeDtypeStruct((blk, width), F32),
            jax.ShapeDtypeStruct((3, blk, width), BF16),
            jax.ShapeDtypeStruct((hosts, 3, 2, width, fh), BF16),
        ),
        in_specs=[vmem] + [anywhere] * 6,
        out_specs=(vmem, anywhere, anywhere),
        scratch_shapes=scratch,
        compiler_params=pltpu.CompilerParams(
            collective_id=0, has_side_effects=True, vmem_limit_bytes=60 * 1024 * 1024
        ),
    )


def solution(mesh):
    groups, ep = mesh.shape["grp"], mesh.shape["ep"]
    across = row_length(mesh)

    def body(
        tokens, norm_gain, expert_ids, gate_weights, expert_gate, expert_up, expert_down,
        shared_gate, shared_up, shared_down, post_gain,
    ):
        blk, width = tokens.shape
        fh = expert_gate.shape[2]
        normed = rms_scale(tokens.astype(F32), norm_gain).astype(BF16)
        experts = jnp.arange(ep, dtype=jnp.int32)[None, None, :]
        table = jnp.sum(jnp.where(expert_ids[:, :, None] == experts, gate_weights[:, :, None], 0.0), axis=1)
        high = lax.reduce_precision(table, 8, 7)
        rest = table - high
        middle = lax.reduce_precision(rest, 8, 7)
        low = rest - middle
        pad = jnp.zeros((blk, 128 - 3 * ep), F32)
        extra = jnp.concatenate([high, middle, low, pad], axis=1).astype(BF16)
        rows = jnp.concatenate([normed, extra], axis=1)
        down = expert_down[0].reshape(fh, width // fh, fh).transpose(1, 0, 2).reshape(width, fh)
        own, back, _ = make_kernel(groups, across, ep, blk, width, fh)(
            rows, expert_gate[0], expert_up[0], down, shared_gate, shared_up, shared_down
        )
        combined = own + jnp.sum(back.astype(F32), axis=0)
        return rms_scale(combined, post_gain).astype(BF16)

    rows_spec = P(("grp", "ep", "tp"), None)
    return jax.shard_map(
        body,
        mesh=mesh,
        in_specs=(
            rows_spec, P(), rows_spec, rows_spec,
            P("ep", None, "tp"), P("ep", None, "tp"), P("ep", "tp", None),
            P(), P(), P(), P(),
        ),
        out_specs=rows_spec,
        check_vma=False,
    )
```

```python
import jax
import jax.numpy as jnp
from jax import lax
from jax.experimental import pallas as pl
from jax.experimental.pallas import tpu as pltpu
from jax.sharding import PartitionSpec as P

EPS = 1e-06
STRIDE = 4
MESH = pl.DeviceIdType.MESH
F32 = jnp.float32
BF16 = jnp.bfloat16


def rms_scale(inputs, gain):
    mean_sq = jnp.mean(inputs * inputs, axis=-1, keepdims=True)
    return inputs * lax.rsqrt(mean_sq + EPS) * gain


def row_length(mesh):
    coords = [getattr(d, "coords", None) for d in mesh.devices.reshape(mesh.devices.shape[0], -1)[:, 0]]
    groups = len(coords)
    if any(c is None for c in coords):
        return 1
    across = len({c[0] for c in coords})
    return across if groups % across == 0 else 1


def silu_mul(g, u):
    return g / (1.0 + jnp.exp(-g)) * u


def dot(a, b):
    return jnp.dot(a, b, preferred_element_type=F32)


def make_kernel(groups, across, ep, blk, width, fh, top):
    hosts = ep // STRIDE
    half = hosts // 2
    share = width // groups
    hb = blk // 2
    chunk = 32
    full_steps = (groups - 1) // 2
    steps = groups // 2
    cuts = [False] * full_steps + [True] * (steps - full_steps)

    def kernel(
        tok_ref, gain_ref, ids_ref, gw_ref, post_ref,
        gate_ref, up_ref, down_ref, sg_ref, su_ref, sd_ref,
        out_ref, wall_ref,
        xs, acc, wb, sgb, sub, sdb, part, inbox, back, hid,
        disp_s, disp_r, rel_s, rel_r, ch_s, ch_r, xy_s, xy_r, dd_s, dd_r, cb_s, cb_r, ld, lw, pace,
    ):
        grp = lax.axis_index("grp")
        z = lax.axis_index("ep")
        core = lax.axis_index("tp")
        other = 1 - core

        def place(g):
            row, col = g // across, g % across
            return row * across + (col if across == 1 else jnp.where(row % 2 == 0, col, across - 1 - col))

        pos = place(grp)
        nxt = place(lax.rem(pos + 1, groups))
        prv = place(lax.rem(pos + groups - 1, groups))

        def zat(d):
            return lax.rem(z + d + ep, ep)

        own_w = (gate_ref, up_ref, wb.at[0, 2, core])
        peers = [{"ep": zat(d)} for d in (1, -1, STRIDE, -STRIDE)]
        peers += [{"tp": other}]
        if groups > 1:
            peers += [{"grp": nxt}, {"grp": prv}]
        barrier = pltpu.get_barrier_semaphore()
        for peer in peers:
            pl.semaphore_signal(barrier, inc=1, device_id=peer, device_id_type=MESH)

        loads = [
            pltpu.make_async_copy(gate_ref, wb.at[0, 0, core], ld.at[0]),
            pltpu.make_async_copy(up_ref, wb.at[0, 1, core], ld.at[1]),
        ]
        for j in range(width // fh):
            cols = slice(j * fh, (j + 1) * fh)
            loads.append(pltpu.make_async_copy(down_ref.at[:, cols], wb.at[0, 2, core, cols], ld.at[2 + j]))
        for i, (a, b) in enumerate(((sg_ref, sgb), (su_ref, sub), (sd_ref, sdb))):
            loads.append(pltpu.make_async_copy(a, b, ld.at[2 + width // fh + i]))
        for load in loads:
            load.start()
        with jax.named_scope("entry"):
            pl.semaphore_wait(barrier, len(peers))

        def remote(src, dst, s, r, to):
            return pltpu.make_async_remote_copy(
                src_ref=src, dst_ref=dst, send_sem=s, recv_sem=r, device_id=to, device_id_type=MESH
            )

        sent = []

        def go(copy):
            copy.start()
            sent.append(copy)

        def dispatch(d, h):
            rows = pl.ds(h * hb, hb)
            return remote(
                xs.at[0, rows], xs.at[1 + d, rows], disp_s.at[d, h], disp_r.at[d, h],
                {"ep": zat(1 - 2 * d)},
            )

        def relay(d):
            rows = pl.ds(d * hb, hb)
            return remote(
                xs.at[1 + d, rows], xs.at[3, rows], rel_s.at[d], rel_r.at[d], {"ep": zat(1 - 2 * d)}
            )

        def slot_of(d, t):
            return t if d == 0 else hosts - t

        def rows_of(region, d, cut):
            if not cut:
                return pl.ds(region * share, share)
            return pl.ds(region * share + d * (share // 2), share // 2)

        def chain(d, m, t):
            rows = rows_of(pos, d, t == half)
            src = own_w[m].at[rows] if t == 1 else wall_ref.at[slot_of(d, t - 1), m, core, rows]
            return remote(
                src, wall_ref.at[slot_of(d, t), m, core, rows], ch_s.at[d, m, t - 1],
                ch_r.at[d, m, t - 1], {"ep": zat(STRIDE * (1 - 2 * d))},
            )

        def exchange(slot, m, j, d, arriving):
            back_by = j if arriving else j - 1
            region = lax.rem(pos + (groups - back_by if d == 0 else back_by), groups)
            ref = wall_ref.at[slot, m, core, rows_of(region, d, cuts[j - 1])]
            return remote(
                ref, ref, xy_s.at[slot, m, j - 1, d], xy_r.at[slot, m, j - 1, d],
                {"grp": nxt if d == 0 else prv},
            )

        def exchange_wait(slots, m, j):
            for slot in slots:
                for d in range(2):
                    exchange(slot, m, j, d, True).wait_recv()

        def exchange_start(slots, m, j):
            for slot in slots:
                for d in range(2):
                    go(exchange(slot, m, j, d, False))

        def swap(slot, m):
            dst = wall_ref.at[slot, m, core]
            src = own_w[m] if slot == 0 else dst
            return remote(src, dst, dd_s.at[slot, m], dd_r.at[slot, m], {"tp": other})

        def finish(slots, m):
            if steps:
                exchange_wait(slots, m, steps)
            for slot in slots:
                go(swap(slot, m))

        for d in range(2):
            go(chain(d, 0, 1))

        lane = lax.broadcasted_iota(jnp.int32, (chunk, 128), 1)

        @pl.loop(0, blk // chunk)
        def _(i):
            rows = pl.ds(pl.multiple_of(i * chunk, chunk), chunk)
            x = tok_ref[rows, :].astype(F32)
            xs[0, rows, :width] = rms_scale(x, gain_ref[...]).astype(BF16)
            table = jnp.zeros((chunk, 128), F32)
            for k in range(top):
                table += jnp.where(ids_ref[rows, k : k + 1] == lane % ep, gw_ref[rows, k : k + 1], 0.0)
            high = table.astype(BF16).astype(F32)
            middle = (table - high).astype(BF16).astype(F32)
            low = table - high - middle
            extra = jnp.where(lane < ep, high, jnp.where(lane < 2 * ep, middle, low))
            xs[0, rows, width:] = jnp.where(lane < 3 * ep, extra, 0.0).astype(BF16)

        for load in loads:
            load.wait()

        x = xs[0, :, :width]
        shared_hidden = silu_mul(dot(x, sgb[...]), dot(x, sub[...])).astype(BF16)

        for h in range(2):
            for d in range(2):
                go(dispatch(d, h if d == 0 else 1 - h))
        for d in range(2):
            go(chain(d, 1, 1))
        for m in range(3):
            go(swap(0, m))
        from_wb = sent[-1:]

        for j in range(width // (2 * fh)):
            cols = slice(j * 2 * fh, (j + 1) * 2 * fh)
            acc[0, :, cols] = dot(shared_hidden, sdb[:, cols])
        for b in range(1, 4):
            acc[b] = jnp.zeros((blk, width), F32)

        order = [0] + [slot_of(d, t) for t in range(1, half) for d in range(2)] + [half]
        turn = {slot: i % 2 for i, slot in enumerate(order)}

        def hidden(slot, b):
            expert = lax.rem(z + ep - STRIDE * slot, ep)
            x = xs[b, :, :width]
            w1 = wb.at[turn[slot]]
            lanes = lax.broadcasted_iota(jnp.int32, (blk, 128), 1)
            pick = (lanes < 3 * ep) & (lanes % ep == expert)
            w = jnp.sum(jnp.where(pick, xs[b, :, width:].astype(F32), 0.0), axis=1, keepdims=True)
            return [(silu_mul(dot(x, w1[0, c]), dot(x, w1[1, c])) * w).astype(BF16) for c in range(2)]

        def down(slot, b, hs, cols):
            w2 = wb.at[turn[slot], 2]
            return acc[b, :, cols] + (dot(hs[0], w2[0, cols, :]) + dot(hs[1], w2[1, cols, :]))

        groups_of_cols = [slice(j * fh, (j + 1) * fh) for j in range(width // fh)]

        def compute(slot):
            @pl.loop(0, 4)
            def _(b):
                hs = hidden(slot, b)
                for cols in groups_of_cols:
                    acc[b, :, cols] = down(slot, b, hs, cols)

        def compute_hidden(slot):
            @pl.loop(0, 4)
            def _(b):
                for c, h in enumerate(hidden(slot, b)):
                    hid[turn[slot], b, c] = h

        def compute_down(slot):
            @pl.loop(0, 4)
            def _(b):
                hs = [hid[turn[slot], b, c] for c in range(2)]
                for cols in groups_of_cols:
                    acc[b, :, cols] = down(slot, b, hs, cols)

        def loading(slot, ms):
            return [
                pltpu.make_async_copy(wall_ref.at[slot, m], wb.at[turn[slot], m], lw.at[turn[slot], m])
                for m in ms
            ]

        def load_start(slot, ms):
            for m in ms:
                swap(slot, m).wait_recv()
            for copy in loading(slot, ms):
                copy.start()

        def load_wait(slot, ms):
            for copy in loading(slot, ms):
                copy.wait()

        def first_slot():
            for m in range(3):
                swap(0, m).wait_recv()
            theirs = [
                pltpu.make_async_copy(wall_ref.at[0, m, other], wb.at[0, m, other], ld.at[m])
                for m in range(3)
            ]
            for load in theirs:
                load.start()
            for d in range(2):
                dispatch(d, 1 - d).wait_recv()
            for d in range(2):
                relay(d).wait_recv()
            for load in theirs:
                load.wait()
            compute(0)

        def advance(slots, m):
            for j in range(2, steps + 1):
                exchange_wait(slots, m, j - 1)
                exchange_start(slots, m, j)

        for d in range(2):
            dispatch(d, d).wait_recv()
            go(relay(d))
        for d in range(2):
            go(chain(d, 2, 1))
        from_wb += sent[-2:]

        last = order[-1]

        def pair_hidden(slots):
            for slot in slots:
                load_start(slot, (0, 1))
            for slot in slots:
                load_wait(slot, (0, 1))
                compute_hidden(slot)

        def pair_down(slots):
            for copy in from_wb:
                copy.wait_send()
                sent[:] = [c for c in sent if c is not copy]
            from_wb.clear()
            for slot in slots:
                load_start(slot, (2,))
            for slot in slots:
                load_wait(slot, (2,))
                compute_down(slot)

        def pace_signal():
            for d in range(2):
                pl.semaphore_signal(pace.at[d], inc=1, device_id={"ep": zat(1 - 2 * d)}, device_id_type=MESH)

        def pace_wait():
            for d in range(2):
                pl.semaphore_wait(pace.at[d], 1)

        previous = None
        for t in range(1, half + 1):
            slots = [slot_of(0, t)] if t == half else [slot_of(0, t), slot_of(1, t)]
            pair = [slot_of(0, t - 1), slot_of(1, t - 1)]
            for m in range(3):
                if previous is not None:
                    with jax.named_scope(f"advance{t}{m}"):
                        advance(*previous)
                with jax.named_scope(f"chain{t}{m}"):
                    for d in range(2):
                        chain(d, m, t).wait_recv()
                with jax.named_scope(f"pace{t}{m}"):
                    pace_signal()
                    if previous is not None:
                        pace_wait()
                if t < half:
                    for d in range(2):
                        go(chain(d, m, t + 1))
                if steps:
                    exchange_start(slots, m, 1)
                with jax.named_scope(f"compute{t}{m}"):
                    if t == 1 and m == 1:
                        first_slot()
                    elif t > 1 and m == 0:
                        pair_hidden(pair)
                    elif t > 1 and m == 1:
                        pair_down(pair)
                if previous is not None:
                    with jax.named_scope(f"finish{t}{m}"):
                        finish(*previous)
                previous = (slots, m)

        pace_wait()
        with jax.named_scope("drain"):
            load_start(last, (0,))
            advance(*previous)
        with jax.named_scope("last_hidden"):
            load_start(last, (1,))
            load_wait(last, (0, 1))
            compute_hidden(last)
        with jax.named_scope("last_finish"):
            finish(*previous)
        with jax.named_scope("last_load"):
            load_start(last, (2,))
            load_wait(last, (2,))

        def combine(i):
            d = i % 2
            early = i < 4
            rows = pl.ds((d if i < 2 or not early else 1 - d) * hb, hb)
            src, dst = (part.at[2, rows], inbox.at[rows]) if i < 2 else (part.at[d, rows], back.at[d, rows])
            return remote(src, dst, cb_s.at[i], cb_r.at[i], {"ep": zat(2 * d - 1)})

        def last_down(b):
            hs = [hid[turn[last], b, c] for c in range(2)]
            for cols in groups_of_cols:
                total = down(last, b, hs, cols)
                if b == 3:
                    part[2, :, cols] = total.astype(BF16)
                elif b == 1:
                    part[0, hb:, cols] = total[hb:].astype(BF16)
                    acc[1, :hb, cols] = total[:hb]
                elif b == 2:
                    part[1, :hb, cols] = total[:hb].astype(BF16)
                    acc[2, hb:, cols] = total[hb:]
                else:
                    acc[0, :, cols] = total

        with jax.named_scope("down31"):
            last_down(3)
            last_down(1)
        with jax.named_scope("send01"):
            go(combine(0))
            go(combine(1))
        with jax.named_scope("down2"):
            last_down(2)
        go(combine(2))
        with jax.named_scope("down0"):
            last_down(0)
        go(combine(3))
        with jax.named_scope("comb0"):
            combine(0).wait_recv()
        with jax.named_scope("add"):
          part[0, :hb, :] = (acc[1, :hb, :] + inbox[:hb, :].astype(F32)).astype(BF16)
        combine(1).wait_recv()
        part[1, hb:, :] = (acc[2, hb:, :] + inbox[hb:, :].astype(F32)).astype(BF16)
        go(combine(4))
        go(combine(5))
        with jax.named_scope("comb"):
            for i in range(2, 6):
                combine(i).wait_recv()

        @pl.loop(0, blk // chunk)
        def _(i):
            rows = pl.ds(pl.multiple_of(i * chunk, chunk), chunk)
            combined = acc[0, rows, :] + back[0, rows, :].astype(F32) + back[1, rows, :].astype(F32)
            out_ref[rows, :] = rms_scale(combined, post_ref[...]).astype(BF16)

        for copy in sent:
            copy.wait_send()

    dma = pltpu.SemaphoreType.DMA
    nsteps = max(steps, 1)
    scratch = [
        pltpu.VMEM((4, blk, width + 128), BF16),
        pltpu.VMEM((4, blk, width), F32),
        pltpu.VMEM((2, 3, 2, width, fh), BF16),
        pltpu.VMEM((width, 2 * fh), BF16),
        pltpu.VMEM((width, 2 * fh), BF16),
        pltpu.VMEM((2 * fh, width), BF16),
        pltpu.VMEM((3, blk, width), BF16),
        pltpu.VMEM((blk, width), BF16),
        pltpu.VMEM((2, blk, width), BF16),
        pltpu.VMEM((2, 4, 2, blk, fh), BF16),
        dma((2, 2)), dma((2, 2)), dma((2,)), dma((2,)),
        dma((2, 3, half)), dma((2, 3, half)),
        dma((hosts, 3, nsteps, 2)), dma((hosts, 3, nsteps, 2)),
        dma((hosts, 3)), dma((hosts, 3)),
        dma((6,)), dma((6,)),
        dma((5 + width // fh,)), dma((2, 3)), pltpu.SemaphoreType.REGULAR((2,)),
    ]
    anywhere = pl.BlockSpec(memory_space=pl.ANY)
    vmem = pl.BlockSpec(memory_space=pltpu.VMEM)
    return pl.pallas_call(
        kernel,
        out_shape=(
            jax.ShapeDtypeStruct((blk, width), BF16),
            jax.ShapeDtypeStruct((hosts, 3, 2, width, fh), BF16),
        ),
        in_specs=[vmem] * 5 + [anywhere] * 6,
        out_specs=(vmem, anywhere),
        scratch_shapes=scratch,
        compiler_params=pltpu.CompilerParams(
            collective_id=0, has_side_effects=True, vmem_limit_bytes=60 * 1024 * 1024
        ),
    )


def solution(mesh):
    groups, ep = mesh.shape["grp"], mesh.shape["ep"]
    across = row_length(mesh)

    def body(
        tokens, norm_gain, expert_ids, gate_weights, expert_gate, expert_up, expert_down,
        shared_gate, shared_up, shared_down, post_gain,
    ):
        blk, width = tokens.shape
        fh = expert_gate.shape[2]
        mixed, _ = make_kernel(groups, across, ep, blk, width, fh, expert_ids.shape[1])(
            tokens, norm_gain[None], expert_ids, gate_weights, post_gain[None],
            expert_gate[0], expert_up[0], expert_down[0], shared_gate, shared_up, shared_down,
        )
        return mixed

    rows_spec = P(("grp", "ep", "tp"), None)
    return jax.shard_map(
        body,
        mesh=mesh,
        in_specs=(
            rows_spec, P(), rows_spec, rows_spec,
            P("ep", None, "tp"), P("ep", None, "tp"), P("ep", "tp", None),
            P(), P(), P(), P(),
        ),
        out_specs=rows_spec,
        check_vma=False,
    )
```

```python
import jax
import jax.numpy as jnp
from jax import lax
from jax.experimental import pallas as pl
from jax.experimental.pallas import tpu as pltpu
from jax.sharding import PartitionSpec as P

EPS = 1e-06
STRIDE = 4
MESH = pl.DeviceIdType.MESH
F32 = jnp.float32
BF16 = jnp.bfloat16


def rms_scale(inputs, gain):
    mean_sq = jnp.mean(inputs * inputs, axis=-1, keepdims=True)
    return inputs * lax.rsqrt(mean_sq + EPS) * gain


def row_length(mesh):
    coords = [getattr(d, "coords", None) for d in mesh.devices.reshape(mesh.devices.shape[0], -1)[:, 0]]
    groups = len(coords)
    if any(c is None for c in coords):
        return 1
    across = len({c[0] for c in coords})
    return across if groups % across == 0 else 1


def silu_mul(g, u):
    return g / (1.0 + jnp.exp(-g)) * u


def dot(a, b):
    return jnp.dot(a, b, preferred_element_type=F32)


def make_kernel(groups, across, ep, blk, width, fh, top):
    hosts = ep // STRIDE
    half = hosts // 2
    share = width // groups
    hb = blk // 2
    chunk = 32
    full_steps = (groups - 1) // 2
    steps = groups // 2
    cuts = [False] * full_steps + [True] * (steps - full_steps)

    def kernel(
        tok_ref, gain_ref, ids_ref, gw_ref, post_ref,
        gate_ref, up_ref, down_ref, sg_ref, su_ref, sd_ref,
        out_ref, wall_ref,
        xs, acc, wb, sgb, sub, sdb, part, inbox, back, hid,
        disp_s, disp_r, rel_s, rel_r, ch_s, ch_r, xy_s, xy_r, dd_s, dd_r, cb_s, cb_r, ld, lw, pace,
    ):
        grp = lax.axis_index("grp")
        z = lax.axis_index("ep")
        core = lax.axis_index("tp")
        other = 1 - core

        def place(g):
            row, col = g // across, g % across
            return row * across + (col if across == 1 else jnp.where(row % 2 == 0, col, across - 1 - col))

        pos = place(grp)
        nxt = place(lax.rem(pos + 1, groups))
        prv = place(lax.rem(pos + groups - 1, groups))

        def zat(d):
            return lax.rem(z + d + ep, ep)

        own_w = (gate_ref, up_ref, wb.at[0, 2, core])
        peers = [{"ep": zat(d)} for d in (1, -1, STRIDE, -STRIDE)]
        peers += [{"tp": other}]
        if groups > 1:
            peers += [{"grp": nxt}, {"grp": prv}]
        barrier = pltpu.get_barrier_semaphore()
        for peer in peers:
            pl.semaphore_signal(barrier, inc=1, device_id=peer, device_id_type=MESH)

        loads = [
            pltpu.make_async_copy(gate_ref, wb.at[0, 0, core], ld.at[0]),
            pltpu.make_async_copy(up_ref, wb.at[0, 1, core], ld.at[1]),
        ]
        for j in range(width // fh):
            cols = slice(j * fh, (j + 1) * fh)
            loads.append(pltpu.make_async_copy(down_ref.at[:, cols], wb.at[0, 2, core, cols], ld.at[2 + j]))
        for i, (a, b) in enumerate(((sg_ref, sgb), (su_ref, sub), (sd_ref, sdb))):
            loads.append(pltpu.make_async_copy(a, b, ld.at[2 + width // fh + i]))
        for load in loads:
            load.start()
        with jax.named_scope("entry"):
            pl.semaphore_wait(barrier, len(peers))

        def remote(src, dst, s, r, to):
            return pltpu.make_async_remote_copy(
                src_ref=src, dst_ref=dst, send_sem=s, recv_sem=r, device_id=to, device_id_type=MESH
            )

        sent = []

        def go(copy):
            copy.start()
            sent.append(copy)

        def dispatch(d, h):
            rows = pl.ds(h * hb, hb)
            return remote(
                xs.at[0, rows], xs.at[1 + d, rows], disp_s.at[d, h], disp_r.at[d, h],
                {"ep": zat(1 - 2 * d)},
            )

        def relay(d):
            rows = pl.ds(d * hb, hb)
            return remote(
                xs.at[1 + d, rows], xs.at[3, rows], rel_s.at[d], rel_r.at[d], {"ep": zat(1 - 2 * d)}
            )

        def slot_of(d, t):
            return t if d == 0 else hosts - t

        def rows_of(region, d, cut):
            if not cut:
                return pl.ds(region * share, share)
            return pl.ds(region * share + d * (share // 2), share // 2)

        def chain(d, m, t):
            rows = rows_of(pos, d, t == half)
            src = own_w[m].at[rows] if t == 1 else wall_ref.at[slot_of(d, t - 1), m, core, rows]
            return remote(
                src, wall_ref.at[slot_of(d, t), m, core, rows], ch_s.at[d, m, t - 1],
                ch_r.at[d, m, t - 1], {"ep": zat(STRIDE * (1 - 2 * d))},
            )

        def exchange(slot, m, j, d, arriving):
            back_by = j if arriving else j - 1
            region = lax.rem(pos + (groups - back_by if d == 0 else back_by), groups)
            ref = wall_ref.at[slot, m, core, rows_of(region, d, cuts[j - 1])]
            return remote(
                ref, ref, xy_s.at[slot, m, j - 1, d], xy_r.at[slot, m, j - 1, d],
                {"grp": nxt if d == 0 else prv},
            )

        def exchange_wait(slots, m, j):
            for slot in slots:
                for d in range(2):
                    exchange(slot, m, j, d, True).wait_recv()

        def exchange_start(slots, m, j):
            for slot in slots:
                for d in range(2):
                    go(exchange(slot, m, j, d, False))

        def swap(slot, m):
            dst = wall_ref.at[slot, m, core]
            src = own_w[m] if slot == 0 else dst
            return remote(src, dst, dd_s.at[slot, m], dd_r.at[slot, m], {"tp": other})

        def finish(slots, m):
            if steps:
                exchange_wait(slots, m, steps)
            for slot in slots:
                go(swap(slot, m))

        for d in range(2):
            go(chain(d, 0, 1))

        lane = lax.broadcasted_iota(jnp.int32, (chunk, 128), 1)

        @pl.loop(0, blk // chunk)
        def _(i):
            rows = pl.ds(pl.multiple_of(i * chunk, chunk), chunk)
            x = tok_ref[rows, :].astype(F32)
            xs[0, rows, :width] = rms_scale(x, gain_ref[...]).astype(BF16)
            table = jnp.zeros((chunk, 128), F32)
            for k in range(top):
                table += jnp.where(ids_ref[rows, k : k + 1] == lane % ep, gw_ref[rows, k : k + 1], 0.0)
            high = table.astype(BF16).astype(F32)
            middle = (table - high).astype(BF16).astype(F32)
            low = table - high - middle
            extra = jnp.where(lane < ep, high, jnp.where(lane < 2 * ep, middle, low))
            xs[0, rows, width:] = jnp.where(lane < 3 * ep, extra, 0.0).astype(BF16)

        for load in loads:
            load.wait()

        x = xs[0, :, :width]
        shared_hidden = silu_mul(dot(x, sgb[...]), dot(x, sub[...])).astype(BF16)

        for h in range(2):
            for d in range(2):
                go(dispatch(d, h if d == 0 else 1 - h))
        for d in range(2):
            go(chain(d, 1, 1))
        for m in range(3):
            go(swap(0, m))
        from_wb = sent[-1:]

        for j in range(width // (2 * fh)):
            cols = slice(j * 2 * fh, (j + 1) * 2 * fh)
            acc[0, :, cols] = dot(shared_hidden, sdb[:, cols])
        for b in range(1, 4):
            acc[b] = jnp.zeros((blk, width), F32)

        order = [0] + [slot_of(d, t) for t in range(1, half) for d in range(2)] + [half]
        turn = {slot: i % 2 for i, slot in enumerate(order)}

        def hidden(slot, b):
            expert = lax.rem(z + ep - STRIDE * slot, ep)
            x = xs[b, :, :width]
            w1 = wb.at[turn[slot]]
            lanes = lax.broadcasted_iota(jnp.int32, (blk, 128), 1)
            pick = (lanes < 3 * ep) & (lanes % ep == expert)
            w = jnp.sum(jnp.where(pick, xs[b, :, width:].astype(F32), 0.0), axis=1, keepdims=True)
            return [(silu_mul(dot(x, w1[0, c]), dot(x, w1[1, c])) * w).astype(BF16) for c in range(2)]

        def down(slot, b, hs, cols):
            w2 = wb.at[turn[slot], 2]
            return acc[b, :, cols] + (dot(hs[0], w2[0, cols, :]) + dot(hs[1], w2[1, cols, :]))

        groups_of_cols = [slice(j * fh, (j + 1) * fh) for j in range(width // fh)]

        def compute(slot):
            @pl.loop(0, 4)
            def _(b):
                hs = hidden(slot, b)
                for cols in groups_of_cols:
                    acc[b, :, cols] = down(slot, b, hs, cols)

        def compute_hidden(slot):
            @pl.loop(0, 4)
            def _(b):
                for c, h in enumerate(hidden(slot, b)):
                    hid[turn[slot], b, c] = h

        def compute_down(slot):
            @pl.loop(0, 4)
            def _(b):
                hs = [hid[turn[slot], b, c] for c in range(2)]
                for cols in groups_of_cols:
                    acc[b, :, cols] = down(slot, b, hs, cols)

        def loading(slot, ms):
            return [
                pltpu.make_async_copy(wall_ref.at[slot, m], wb.at[turn[slot], m], lw.at[turn[slot], m])
                for m in ms
            ]

        def load_start(slot, ms):
            for m in ms:
                swap(slot, m).wait_recv()
            for copy in loading(slot, ms):
                copy.start()

        def load_wait(slot, ms):
            for copy in loading(slot, ms):
                copy.wait()

        def first_slot():
            for m in range(3):
                swap(0, m).wait_recv()
            theirs = [
                pltpu.make_async_copy(wall_ref.at[0, m, other], wb.at[0, m, other], ld.at[m])
                for m in range(3)
            ]
            for load in theirs:
                load.start()
            for d in range(2):
                dispatch(d, 1 - d).wait_recv()
            for d in range(2):
                relay(d).wait_recv()
            for load in theirs:
                load.wait()
            compute(0)

        def advance(slots, m):
            for j in range(2, steps + 1):
                exchange_wait(slots, m, j - 1)
                exchange_start(slots, m, j)

        for d in range(2):
            dispatch(d, d).wait_recv()
            go(relay(d))
        for d in range(2):
            go(chain(d, 2, 1))
        from_wb += sent[-2:]

        last = order[-1]

        def pair_hidden(slots):
            for slot in slots:
                load_start(slot, (0, 1))
            for slot in slots:
                load_wait(slot, (0, 1))
                compute_hidden(slot)

        def pair_down(slots):
            for copy in from_wb:
                copy.wait_send()
                sent[:] = [c for c in sent if c is not copy]
            from_wb.clear()
            for slot in slots:
                load_start(slot, (2,))
            for slot in slots:
                load_wait(slot, (2,))
                compute_down(slot)

        def pace_signal():
            for d in range(2):
                pl.semaphore_signal(pace.at[d], inc=1, device_id={"ep": zat(1 - 2 * d)}, device_id_type=MESH)

        def pace_wait():
            for d in range(2):
                pl.semaphore_wait(pace.at[d], 1)

        previous = None
        for t in range(1, half + 1):
            slots = [slot_of(0, t)] if t == half else [slot_of(0, t), slot_of(1, t)]
            pair = [slot_of(0, t - 1), slot_of(1, t - 1)]
            for m in range(3):
                if previous is not None:
                    with jax.named_scope(f"advance{t}{m}"):
                        advance(*previous)
                with jax.named_scope(f"chain{t}{m}"):
                    for d in range(2):
                        chain(d, m, t).wait_recv()
                with jax.named_scope(f"pace{t}{m}"):
                    pace_signal()
                    if previous is not None:
                        pace_wait()
                if t < half and (t, m) != (1, 0):
                    for late in (0, 1) if (t, m) == (1, 1) else (m,):
                        for d in range(2):
                            go(chain(d, late, t + 1))
                if steps:
                    exchange_start(slots, m, 1)
                with jax.named_scope(f"compute{t}{m}"):
                    if t == 1 and m == 1:
                        first_slot()
                    elif t > 1 and m == 0:
                        pair_hidden(pair)
                    elif t > 1 and m == 1:
                        pair_down(pair)
                if previous is not None:
                    with jax.named_scope(f"finish{t}{m}"):
                        finish(*previous)
                previous = (slots, m)

        pace_wait()
        with jax.named_scope("drain"):
            load_start(last, (0,))
            advance(*previous)
        with jax.named_scope("last_hidden"):
            load_start(last, (1,))
            load_wait(last, (0, 1))
            compute_hidden(last)
        with jax.named_scope("last_finish"):
            finish(*previous)
        with jax.named_scope("last_load"):
            load_start(last, (2,))
            load_wait(last, (2,))

        def combine(i):
            d = i % 2
            early = i < 4
            rows = pl.ds((d if i < 2 or not early else 1 - d) * hb, hb)
            src, dst = (part.at[2, rows], inbox.at[rows]) if i < 2 else (part.at[d, rows], back.at[d, rows])
            return remote(src, dst, cb_s.at[i], cb_r.at[i], {"ep": zat(2 * d - 1)})

        def last_down(b):
            hs = [hid[turn[last], b, c] for c in range(2)]
            for cols in groups_of_cols:
                total = down(last, b, hs, cols)
                if b == 3:
                    part[2, :, cols] = total.astype(BF16)
                elif b == 1:
                    part[0, hb:, cols] = total[hb:].astype(BF16)
                    acc[1, :hb, cols] = total[:hb]
                elif b == 2:
                    part[1, :hb, cols] = total[:hb].astype(BF16)
                    acc[2, hb:, cols] = total[hb:]
                else:
                    acc[0, :, cols] = total

        with jax.named_scope("down31"):
            last_down(3)
            last_down(1)
        with jax.named_scope("send01"):
            go(combine(0))
            go(combine(1))
        with jax.named_scope("down2"):
            last_down(2)
        go(combine(2))
        with jax.named_scope("down0"):
            last_down(0)
        go(combine(3))
        with jax.named_scope("comb0"):
            combine(0).wait_recv()
        with jax.named_scope("add"):
            part[0, :hb, :] = (acc[1, :hb, :] + inbox[:hb, :].astype(F32)).astype(BF16)
        combine(1).wait_recv()
        part[1, hb:, :] = (acc[2, hb:, :] + inbox[hb:, :].astype(F32)).astype(BF16)
        go(combine(4))
        go(combine(5))
        with jax.named_scope("comb"):
            for i in range(2, 6):
                combine(i).wait_recv()

        @pl.loop(0, blk // chunk)
        def _(i):
            rows = pl.ds(pl.multiple_of(i * chunk, chunk), chunk)
            combined = acc[0, rows, :] + back[0, rows, :].astype(F32) + back[1, rows, :].astype(F32)
            out_ref[rows, :] = rms_scale(combined, post_ref[...]).astype(BF16)

        for copy in sent:
            copy.wait_send()

    dma = pltpu.SemaphoreType.DMA
    nsteps = max(steps, 1)
    scratch = [
        pltpu.VMEM((4, blk, width + 128), BF16),
        pltpu.VMEM((4, blk, width), F32),
        pltpu.VMEM((2, 3, 2, width, fh), BF16),
        pltpu.VMEM((width, 2 * fh), BF16),
        pltpu.VMEM((width, 2 * fh), BF16),
        pltpu.VMEM((2 * fh, width), BF16),
        pltpu.VMEM((3, blk, width), BF16),
        pltpu.VMEM((blk, width), BF16),
        pltpu.VMEM((2, blk, width), BF16),
        pltpu.VMEM((2, 4, 2, blk, fh), BF16),
        dma((2, 2)), dma((2, 2)), dma((2,)), dma((2,)),
        dma((2, 3, half)), dma((2, 3, half)),
        dma((hosts, 3, nsteps, 2)), dma((hosts, 3, nsteps, 2)),
        dma((hosts, 3)), dma((hosts, 3)),
        dma((6,)), dma((6,)),
        dma((5 + width // fh,)), dma((2, 3)), pltpu.SemaphoreType.REGULAR((2,)),
    ]
    anywhere = pl.BlockSpec(memory_space=pl.ANY)
    vmem = pl.BlockSpec(memory_space=pltpu.VMEM)
    return pl.pallas_call(
        kernel,
        out_shape=(
            jax.ShapeDtypeStruct((blk, width), BF16),
            jax.ShapeDtypeStruct((hosts, 3, 2, width, fh), BF16),
        ),
        in_specs=[vmem] * 5 + [anywhere] * 6,
        out_specs=(vmem, anywhere),
        scratch_shapes=scratch,
        compiler_params=pltpu.CompilerParams(
            collective_id=0, has_side_effects=True, vmem_limit_bytes=60 * 1024 * 1024
        ),
    )


def solution(mesh):
    groups, ep = mesh.shape["grp"], mesh.shape["ep"]
    across = row_length(mesh)

    def body(
        tokens, norm_gain, expert_ids, gate_weights, expert_gate, expert_up, expert_down,
        shared_gate, shared_up, shared_down, post_gain,
    ):
        blk, width = tokens.shape
        fh = expert_gate.shape[2]
        mixed, _ = make_kernel(groups, across, ep, blk, width, fh, expert_ids.shape[1])(
            tokens, norm_gain[None], expert_ids, gate_weights, post_gain[None],
            expert_gate[0], expert_up[0], expert_down[0], shared_gate, shared_up, shared_down,
        )
        return mixed

    rows_spec = P(("grp", "ep", "tp"), None)
    return jax.shard_map(
        body,
        mesh=mesh,
        in_specs=(
            rows_spec, P(), rows_spec, rows_spec,
            P("ep", None, "tp"), P("ep", None, "tp"), P("ep", "tp", None),
            P(), P(), P(), P(),
        ),
        out_specs=rows_spec,
        check_vma=False,
    )
```
